256 devices in a mesh: sp: 64 (over z, y, core), tp: 4 (over x).
Axes of the slice: x: 4, y: 4, z: 8, core: 2. Of those that a mesh axis runs over, the one named last changes fastest.
Arguments:
- query_proj: bfloat16 [16384, 2048], P('sp', 'tp'), may hold values from -240 to 240
- key_projection: bfloat16 [16384, 512], P('sp', 'tp'), may hold values from -6 to 6
- value_projection: bfloat16 [16384, 512], P('sp', 'tp'), may hold values from -6 to 6
- sink_logit: float32 [32], P('tp'), may hold values from 1 to 6
- residual: bfloat16 [16384, 2048], P('sp'), may hold values from -3 to 3
- w_out: bfloat16 [2048, 2048], P('tp'), may hold values from -1 to 1
- norm_gain: float32 [2048], replicated, may hold values from 0.1 to 1.9
- routes: int32 [16384, 2], P('sp'), may hold values from 0 to 63, all different within a row; in each aligned block of 256 rows (0 to 255, 256 to 511, ...) at most 16 rows name the same one
- route_weights: float32 [16384, 2], P('sp'), may hold values from 0.1 to 1
- w_gate: bfloat16 [64, 2048, 2560], P('sp', None, 'tp'), may hold values from -0.125 to 0.125
- w_up: bfloat16 [64, 2048, 2560], P('sp', None, 'tp'), may hold values from -0.125 to 0.125
- w_down: bfloat16 [64, 2560, 2048], P('sp', 'tp'), may hold values from -0.125 to 0.125
Outputs:
- layer_out: bfloat16 [16384, 2048], P('sp', 'tp')
The draws below stay inside these ranges and needn't reach their ends.
Inputs may be any that keep to these rules, and one draw needn't show every extreme that they name: `routes`: within the rows of one index of sp (aligned blocks of 256 tokens), no expert is named more than 16 times, and in some block one expert is named exactly 16 times. The two experts of a token differ.
All inputs are finite; a program needn't handle non-finite values.
Results may differ from the reference program's by a relative error of at most 0.015.
Values may be sent and summed in bfloat16 or wider, within the bound.
No kernel may reach another device: no remote copies, remote signals or barrier semaphores. Data moves between devices by JAX's collectives and lax.ppermute only.
A program may use at most 64 MiB of HBM per device.

```python
import math
import jax
import jax.numpy as jnp
import numpy as np
from jax import lax

D = 2048
QUERY_HEADS = 32
KEY_VALUE_HEADS = 8
HEAD_SIZE = 64
WINDOW = 128
GRID_W = 64
EF = 2560
TOP = 2
TOK_DEV = 256
SEQUENCE_TOKENS = 16384
EXPERTS = 64
CAP = 16
WIDTH_BLOCKS = 4
N_SP = 64


def drawn_pair(key):
    unrotated_keys = jnp.clip(jax.random.normal(jax.random.fold_in(key, 11), (SEQUENCE_TOKENS, KEY_VALUE_HEADS, HEAD_SIZE), jnp.float32), -6.0, 6.0)
    unrotated_queries = jnp.clip(jax.random.normal(jax.random.fold_in(key, 12), (SEQUENCE_TOKENS, QUERY_HEADS, HEAD_SIZE), jnp.float32), -6.0, 6.0)
    return (unrotated_queries.reshape(SEQUENCE_TOKENS, QUERY_HEADS * HEAD_SIZE), unrotated_keys.reshape(SEQUENCE_TOKENS, KEY_VALUE_HEADS * HEAD_SIZE))


def draw_query_proj(key, part):
    return drawn_pair(key)[0].astype(jnp.bfloat16)


def draw_key_projection(key, part):
    return drawn_pair(key)[1].astype(jnp.bfloat16)


def block_scale(rng, extent, cuts, low, top_value):
    loudness, own = 1.0, jax.random.fold_in(rng, 6)
    for dim, parts in cuts:
        heights = jnp.exp(jax.random.uniform(jax.random.fold_in(own, dim), (parts,), jnp.float32, low / len(cuts), top_value / len(cuts)))
        loudness = loudness * jnp.repeat(heights, extent[dim] // parts).reshape([-1 if axis == dim else 1 for axis in range(len(extent))])
    return loudness


def routed_block(rng, own, number, rows, count, top, most, lean):
    order = jax.random.permutation(rng, count)
    crowded, usual = portions_of(count, rows * top, most, lean, True), portions_of(count, rows * top, most, lean, False)
    places = jnp.arange(count)

    def named(sizes, turn):
        used = int((sizes > 0).sum())
        fixed = max(1, used // 4)
        moved = fixed + (places - fixed + turn * (used - fixed)) % max(1, count - fixed)
        return jnp.zeros((count,), jnp.int32).at[order[jnp.where(places < fixed, places, moved)]].set(jnp.asarray(sizes, jnp.int32))

    sizes = jnp.where(number % 4 == 0, named(crowded, number // 4), named(usual, number - number // 4 - 1))
    mixed = jax.random.permutation(jax.random.fold_in(own, 3), count)
    giver, taker = mixed[0:count // 2 * 2:2], mixed[1:count // 2 * 2:2]
    margin = jnp.minimum(sizes[giver] - 1, most - sizes[taker]) // 2
    margin = jnp.where((giver == order[0]) | (taker == order[0]) | (sizes[taker] == 0), 0, jnp.maximum(margin, 0))
    moved = jax.random.randint(jax.random.fold_in(own, 4), (count // 2,), 0, 1 << 20) % (margin + 1)
    sizes = sizes.at[giver].add(-moved).at[taker].add(moved)
    items = jnp.searchsorted(jnp.cumsum(sizes), jnp.arange(rows * top), side="right").astype(jnp.int32)
    listing = items.reshape(top, rows).T
    listing = listing[jax.random.permutation(jax.random.fold_in(own, 1), rows)]
    turn = jax.random.randint(jax.random.fold_in(own, 2), (rows, 1), 0, top)
    return jnp.take_along_axis(listing, (jnp.arange(top)[None, :] + turn) % top, axis=1)


def portions_of(amount, total, limit, lean, full):
    loads = [(1 << 20) // math.isqrt(grade ** lean) + 1 for grade in range(1, amount + 1)]
    largest = limit if full else min(limit, max(-(-total // amount), total * loads[0] // sum(loads)))
    least = 1 if total - largest >= amount - 1 else 0
    counts, rest = [largest] + [least] * (amount - 1), total - largest - least * (amount - 1)
    while rest > 0:
        free = [i for i in range(1, amount) if counts[i] < largest] or [i for i in range(1, amount) if counts[i] < limit]
        mass, budget = sum([loads[i] for i in free]), rest
        for i in free:
            extra = min(limit - counts[i], max(1, budget * loads[i] // mass), rest)
            counts[i] = counts[i] + extra
            rest = rest - extra
    return np.array(counts)


def scatter_about(key, dims, spread, reach, cuts=(), held_as=jnp.bfloat16):
    loudness = block_scale(key, dims, cuts, -0.22, 0.18) if cuts else 1.0
    array = jax.random.normal(key, dims, jnp.float32) * spread * loudness
    return jnp.minimum(jnp.maximum(array, -reach), reach).astype(held_as)


def setup_inputs(seed: int = 0) -> dict:
    key_list = jax.random.split(jax.random.key(seed), 13)
    query_proj = draw_query_proj(jax.random.fold_in(key_list[12], 71), 0)
    key_projection = draw_key_projection(jax.random.fold_in(key_list[12], 71), 0)
    value_projection = scatter_about(key_list[2], (SEQUENCE_TOKENS, KEY_VALUE_HEADS * HEAD_SIZE), 1.0, 6.0, ((0, 64), (1, 4)))
    sink_logit = jnp.clip(1.0 + 5.0 * jax.random.uniform(key_list[3], (QUERY_HEADS,), jnp.float32) ** block_scale(key_list[3], (QUERY_HEADS,), ((0, 4),), -0.2, 0.2), 1.0, 6.0)
    residual = scatter_about(key_list[4], (SEQUENCE_TOKENS, D), 0.5, 3.0, ((0, 64),))
    w_out = scatter_about(key_list[5], (QUERY_HEADS * HEAD_SIZE, D), (QUERY_HEADS * HEAD_SIZE // 64) ** -0.5, 1.0, ((0, 4),))
    norm_gain = jnp.clip(1.0 + 0.18 * jax.random.normal(key_list[6], (D,), jnp.float32), 0.1, 1.9)
    routes_keys = jax.random.split(jax.random.fold_in(key_list[7], 1), SEQUENCE_TOKENS // TOK_DEV)
    routes_turns = jax.random.permutation(jax.random.fold_in(key_list[7], 3), SEQUENCE_TOKENS // TOK_DEV)
    routes = jax.vmap(lambda own, number: routed_block(jax.random.fold_in(key_list[7], 2), own, number, TOK_DEV, EXPERTS, TOP, CAP, 2))(routes_keys, routes_turns).reshape((SEQUENCE_TOKENS, TOP))
    route_weights = jnp.clip(jnp.exp(math.log(1.0) - 2.3025851 * jax.random.uniform(key_list[8], (SEQUENCE_TOKENS, TOP), jnp.float32) ** block_scale(key_list[8], (SEQUENCE_TOKENS, TOP), ((0, 64),), -0.2, 0.2)), 0.1, 1.0)
    w_gate = scatter_about(key_list[9], (EXPERTS, D, EF), D ** -0.5, 0.125, ((0, 64), (2, 4)))
    w_up = scatter_about(key_list[10], (EXPERTS, D, EF), D ** -0.5, 0.125, ((0, 64), (2, 4)))
    w_down = scatter_about(key_list[11], (EXPERTS, EF, D), EF ** -0.5, 0.125, ((0, 64), (1, 4)))
    return dict(query_proj=query_proj, key_projection=key_projection, value_projection=value_projection, sink_logit=sink_logit, residual=residual, w_out=w_out, norm_gain=norm_gain, routes=routes, route_weights=route_weights, w_gate=w_gate, w_up=w_up, w_down=w_down)


ROPE_BASE = 10000.0
NORM_EPS = 1e-06

def rotate_pair(values_half, angles):
    first_half, second = jnp.split(values_half, 2, axis=-1)
    cosine = jnp.cos(angles)[:, None, :]
    sine_part = jnp.sin(angles)[:, None, :]
    return jnp.concatenate([first_half * cosine - second * sine_part, second * cosine + first_half * sine_part], axis=-1)

def axial_rotation(heads_in, token_positions):
    half_dim = HEAD_SIZE // 2
    inverse = ROPE_BASE ** (-jnp.arange(0, half_dim, 2, dtype=jnp.float32) / half_dim)
    row_angles = (token_positions // GRID_W).astype(jnp.float32)[:, None] * inverse
    col_angles = (token_positions % GRID_W).astype(jnp.float32)[:, None] * inverse
    as_float = heads_in.astype(jnp.float32)
    return jnp.concatenate([rotate_pair(as_float[..., :half_dim], row_angles), rotate_pair(as_float[..., half_dim:], col_angles)], axis=-1)

def attend_block(query_rows, key_rows, value_rows, sink_logit, query_pos, key_pos, total_rows):
    kv_heads = key_rows.shape[1]
    groups = query_rows.shape[1] // kv_heads
    grouped = query_rows.reshape(query_rows.shape[0], kv_heads, groups, HEAD_SIZE).astype(jnp.float32)
    scores = jnp.einsum('qkgd,jkd->kgqj', grouped, key_rows.astype(jnp.float32)) * HEAD_SIZE ** (-0.5)
    in_window = (jnp.abs(key_pos[None, :] - query_pos[:, None]) <= WINDOW) & (key_pos[None, :] >= 0) & (key_pos[None, :] < total_rows)
    scores = jnp.where(in_window[None, None], scores, -jnp.inf)
    sink_col = sink_logit.astype(jnp.float32).reshape(kv_heads, groups, 1, 1)
    largest = jnp.maximum(lax.optimization_barrier(jnp.max(scores, axis=-1, keepdims=True)), sink_col)
    exp_scores = jnp.exp(scores - largest)
    denominator = lax.optimization_barrier(jnp.sum(exp_scores, axis=-1, keepdims=True)) + jnp.exp(sink_col - largest)
    weights_bf = (exp_scores / denominator).astype(jnp.bfloat16)
    mixed_heads = jnp.einsum('kgqj,jkd->qkgd', weights_bf.astype(jnp.float32), value_rows.astype(jnp.float32))
    return mixed_heads.astype(jnp.bfloat16).reshape(query_rows.shape[0], -1)

def blocked_product(left, right, blocks_count):
    part_width = left.shape[1] // blocks_count
    accumulated = jnp.zeros((left.shape[0], right.shape[1]), jnp.float32)
    for block_number in range(blocks_count):
        partial_term = jnp.dot(left[:, block_number * part_width:(block_number + 1) * part_width], right[block_number * part_width:(block_number + 1) * part_width], preferred_element_type=jnp.float32).astype(jnp.bfloat16)
        accumulated = accumulated + lax.optimization_barrier(partial_term).astype(jnp.float32)
    return accumulated

def reference(query_proj, key_projection, value_projection, sink_logit, residual, w_out, norm_gain, routes, route_weights, w_gate, w_up, w_down):
    token_positions = jnp.arange(SEQUENCE_TOKENS, dtype=jnp.int32)
    rot_q = axial_rotation(query_proj.reshape(SEQUENCE_TOKENS, QUERY_HEADS, HEAD_SIZE), token_positions).astype(jnp.bfloat16)
    rotated_keys = axial_rotation(key_projection.reshape(SEQUENCE_TOKENS, KEY_VALUE_HEADS, HEAD_SIZE), token_positions).astype(jnp.bfloat16)
    value_head_rows = value_projection.reshape(SEQUENCE_TOKENS, KEY_VALUE_HEADS, HEAD_SIZE)
    pad_keys = jnp.pad(rotated_keys, ((WINDOW, WINDOW), (0, 0), (0, 0)))
    pad_values = jnp.pad(value_head_rows, ((WINDOW, WINDOW), (0, 0), (0, 0)))

    def one_block(block_index):
        block_start = (block_index * TOK_DEV).astype(jnp.int32)
        query_rows = lax.dynamic_slice_in_dim(rot_q, block_start, TOK_DEV, 0)
        key_rows = lax.dynamic_slice_in_dim(pad_keys, block_start, TOK_DEV + 2 * WINDOW, 0)
        value_rows = lax.dynamic_slice_in_dim(pad_values, block_start, TOK_DEV + 2 * WINDOW, 0)
        query_pos = block_start + jnp.arange(TOK_DEV, dtype=jnp.int32)
        key_pos = block_start - WINDOW + jnp.arange(TOK_DEV + 2 * WINDOW, dtype=jnp.int32)
        return attend_block(query_rows, key_rows, value_rows, sink_logit, query_pos, key_pos, SEQUENCE_TOKENS)
    attended = lax.map(one_block, jnp.arange(SEQUENCE_TOKENS // TOK_DEV, dtype=jnp.int32)).reshape(SEQUENCE_TOKENS, QUERY_HEADS * HEAD_SIZE)
    summed = blocked_product(attended, w_out, WIDTH_BLOCKS)
    stream = (residual.astype(jnp.float32) + summed).astype(jnp.bfloat16)
    as_float = stream.astype(jnp.float32)
    normed = (as_float * lax.rsqrt(lax.optimization_barrier(jnp.mean(as_float * as_float, axis=-1, keepdims=True)) + NORM_EPS) * norm_gain).astype(jnp.bfloat16)
    flat_routes = routes.reshape(N_SP, TOK_DEV * TOP)
    onehot = (flat_routes[:, :, None] == jnp.arange(EXPERTS, dtype=jnp.int32)[None, None, :]).astype(jnp.int32)
    slot_number = lax.optimization_barrier(jnp.sum(jnp.cumsum(onehot, axis=1) * onehot, axis=2)) - 1
    source = jnp.arange(N_SP, dtype=jnp.int32)[:, None]
    destination = (flat_routes * (N_SP * CAP) + source * CAP + slot_number).reshape(-1).astype(jnp.int32)
    copies = jnp.repeat(normed, TOP, axis=0)
    buffer = jnp.zeros((EXPERTS * N_SP * CAP, D), jnp.bfloat16).at[destination].set(copies)
    buffer = buffer.reshape(EXPERTS, N_SP * CAP, D)

    def expert(operands):
        expert_rows, gate_weight, up_weight, down_weight = operands
        gate_part = jnp.dot(expert_rows, gate_weight, preferred_element_type=jnp.float32)
        up_part = jnp.dot(expert_rows, up_weight, preferred_element_type=jnp.float32)
        hidden = (jax.nn.silu(gate_part) * up_part).astype(jnp.bfloat16)
        return blocked_product(hidden, down_weight, WIDTH_BLOCKS).astype(jnp.bfloat16)
    outputs = lax.map(expert, (buffer, w_gate, w_up, w_down)).reshape(-1, D)
    picked = outputs[destination].astype(jnp.float32).reshape(SEQUENCE_TOKENS, TOP, D)
    mixture = lax.optimization_barrier(jnp.sum(picked * route_weights[:, :, None], axis=1))
    return (stream.astype(jnp.float32) + mixture).astype(jnp.bfloat16)
```

```python
import functools

import jax
import jax.numpy as jnp
import numpy as np
from jax import lax
from jax.experimental import pallas as pl
from jax.experimental.pallas import tpu as pltpu
from jax.sharding import PartitionSpec as P

HEAD_SIZE = 64
WINDOW = 128
GRID_W = 64
ROPE_BASE = 10000.0
NORM_EPS = 1e-06
CHUNKS = ((0, 8), (8, 16))


BF16, F32 = jnp.bfloat16, jnp.float32
VMEM = pl.BlockSpec(memory_space=pltpu.VMEM)
SMEM = pl.BlockSpec(memory_space=pltpu.SMEM)


def dot(a, b, dims=((1,), (0,))):
    return lax.dot_general(a, b, (dims, ((), ())), preferred_element_type=F32)


def call(body, outs, ins, flops, name, scratch=(), limit=48 << 20):
    nbytes = sum(int(np.prod(o.shape)) * o.dtype.itemsize for o in outs)
    return pl.pallas_call(
        body,
        out_shape=outs,
        in_specs=ins,
        out_specs=[VMEM] * len(outs),
        scratch_shapes=scratch,
        name=name,
        cost_estimate=pl.CostEstimate(
            flops=flops, bytes_accessed=2 * nbytes, transcendentals=0
        ),
        compiler_params=pltpu.CompilerParams(vmem_limit_bytes=limit),
    )


def angle_tables(seq_devices, tok_rows):
    half = HEAD_SIZE // 2
    inverse = ROPE_BASE ** (-np.arange(0, half, 2, dtype=np.float64) / half)
    lanes = np.arange(2 * HEAD_SIZE) % HEAD_SIZE
    freq = inverse[lanes % (half // 2)].astype(np.float32)
    is_row = lanes < half
    per = tok_rows // GRID_W
    halo = WINDOW // GRID_W
    rows = np.arange(seq_devices)[:, None] * per + np.arange(-halo, per + halo)[None]
    row_angle = rows.astype(np.float32)[..., None] * freq
    col_angle = np.arange(GRID_W, dtype=np.float32)[:, None] * freq
    tables = []
    for fn in (np.cos, np.sin):
        row = np.where(is_row, fn(row_angle.astype(np.float64)), 0.0)
        col = np.where(is_row, 0.0, fn(col_angle.astype(np.float64)))
        tables.append((row.astype(np.float32), col.astype(np.float32)))
    return tables


def edges_body(k_ref, v_ref, tail_ref, head_ref):
    rows, width = k_ref.shape
    tail_ref[:, :width] = k_ref[rows - WINDOW :, :]
    tail_ref[:, width:] = v_ref[rows - WINDOW :, :]
    head_ref[:, :width] = k_ref[:WINDOW, :]
    head_ref[:, width:] = v_ref[:WINDOW, :]


def attention_body(
    ids_ref, sink_ref, q_ref, k_ref, v_ref, left_ref, right_ref,
    rowc_ref, rows_ref, colc_ref, cols_ref, w_ref,
    p2a_ref, p2b_ref, pra_ref, prb_ref, pla_ref, plb_ref, po_ref,
    cos_ref, sin_ref, kd_ref, vd_ref, att_ref, *, seq_devices,
):
    sp, tp = ids_ref[0], ids_ref[1]
    tok = q_ref.shape[0]
    lanes = 2 * HEAD_SIZE
    span = tok + 2 * WINDOW
    row_cos, row_sin = rowc_ref[sp], rows_ref[sp]
    for r in range(span // GRID_W):
        at = pl.ds(r * GRID_W, GRID_W)
        cos_ref[at, :] = row_cos[r : r + 1, :] + colc_ref[...]
        sin_ref[at, :] = row_sin[r : r + 1, :] + cols_ref[...]
    quarter = HEAD_SIZE // 4
    i = lax.broadcasted_iota(jnp.int32, (lanes, lanes), 0)
    j = lax.broadcasted_iota(jnp.int32, (lanes, lanes), 1)
    first = (j % (2 * quarter)) < quarter
    swap = jnp.where(
        first & (i == j + quarter), -1.0, jnp.where(~first & (i == j - quarter), 1.0, 0.0)
    ).astype(BF16)

    def rotated(x, start):
        at = pl.ds(start, x.shape[0])
        return (x.astype(F32) * cos_ref[at, :] + dot(x, swap) * sin_ref[at, :]).astype(BF16)

    pieces = (
        (0, left_ref[:, :lanes], left_ref[:, lanes:]),
        (WINDOW, k_ref[...], v_ref[...]),
        (WINDOW + tok, right_ref[:, :lanes], right_ref[:, lanes:]),
    )
    for g in range(2):
        spread = (i == (j % HEAD_SIZE) + g * HEAD_SIZE).astype(BF16)
        for start, keys, values in pieces:
            at = pl.ds(start, keys.shape[0])
            kd_ref[g, at, :] = dot(rotated(keys, start), spread).astype(BF16)
            vd_ref[g, at, :] = dot(values, spread).astype(BF16)

    reach = 3 * WINDOW
    qi = lax.broadcasted_iota(jnp.int32, (2 * WINDOW, reach), 0) % WINDOW
    kj = lax.broadcasted_iota(jnp.int32, (2 * WINDOW, reach), 1)
    near = (kj >= qi) & (kj - qi <= 2 * WINDOW)
    low = lax.broadcasted_iota(jnp.int32, (WINDOW, lanes), 1) < HEAD_SIZE
    upper = lax.broadcasted_iota(jnp.int32, (2 * WINDOW, 1), 0) < WINDOW
    scale = HEAD_SIZE ** (-0.5)
    for b in range(tok // WINDOW):
        key_pos = sp * tok + (b - 1) * WINDOW + kj
        keep = near & (key_pos >= 0) & (key_pos < seq_devices * tok)
        for p in range(q_ref.shape[1] // lanes):
            g = p // 2
            q = rotated(q_ref[pl.ds(b * WINDOW, WINDOW), pl.ds(p * lanes, lanes)], (b + 1) * WINDOW)
            zero = jnp.zeros_like(q)
            both = jnp.concatenate([jnp.where(low, q, zero), jnp.where(low, zero, q)], axis=0)
            keys = kd_ref[g, pl.ds(b * WINDOW, reach), :]
            scores = dot(both, keys, ((1,), (1,))) * scale
            scores = jnp.where(keep, scores, -jnp.inf)
            sink = jnp.where(upper, sink_ref[2 * p], sink_ref[2 * p + 1])
            most = jnp.maximum(jnp.max(scores, axis=1, keepdims=True), sink)
            e = jnp.exp(scores - most)
            total = jnp.sum(e, axis=1, keepdims=True) + jnp.exp(sink - most)
            probs = (e * (1.0 / total)).astype(BF16)
            mixed = dot(probs, vd_ref[g, pl.ds(b * WINDOW, reach), :])
            att_ref[pl.ds(b * WINDOW, WINDOW), pl.ds(p * lanes, lanes)] = jnp.where(
                low, mixed[:WINDOW], mixed[WINDOW:]
            ).astype(BF16)

    width = po_ref.shape[1]
    half = tok // 2
    att = att_ref[...]

    def partial(step):
        col = pl.multiple_of(lax.rem(tp + step, 4) * width, width)
        return dot(att, w_ref[:, pl.ds(col, width)]).astype(BF16)

    across = partial(2)
    p2a_ref[...], p2b_ref[...] = across[:half], across[half:]
    right = partial(1)
    pra_ref[...], prb_ref[...] = right[:half], right[half:]
    left = partial(3)
    pla_ref[...], plb_ref[...] = left[:half], left[half:]
    po_ref[...] = partial(0)


def dispatch_body(res_ref, po_ref, ra_ref, rb_ref, la_ref, lb_ref, dest_ref, stream_ref, *outs):
    half = ra_ref.shape[0]
    for k, (r, l) in enumerate(((ra_ref, la_ref), (rb_ref, lb_ref))):
        at = pl.ds(k * half, half)
        total = po_ref[at, :].astype(F32) + r[...].astype(F32) + l[...].astype(F32)
        stream_ref[at, :] = (res_ref[at, :].astype(F32) + total).astype(BF16)
    stream = stream_ref[...]
    tok = stream.shape[0]
    for k, out in enumerate(outs):
        rows = out.shape[0]
        at = lax.broadcasted_iota(jnp.int32, (rows, tok), 0)
        d0, d1 = dest_ref[2 * k : 2 * k + 1, :], dest_ref[2 * k + 1 : 2 * k + 2, :]
        pick = jnp.where((at == d0) | (at == d1), 1.0, 0.0).astype(BF16)
        out[...] = dot(pick, stream).astype(BF16)


def expert_body(
    ids_ref, own_ref, r_ref, l_ref, o_ref, gain_ref, wg_ref, wu_ref, wd_ref,
    p2_ref, pr_ref, pl_ref, po_ref, xn_ref, *, block,
):
    tp = ids_ref[1]
    rows, width = own_ref.shape
    full = 4 * width
    parts = ((own_ref, 0), (r_ref, 3), (l_ref, 1), (o_ref, 2))

    def col(step):
        return pl.ds(pl.multiple_of(lax.rem(tp + step, 4) * width, width), width)

    def one(n, _):
        at = pl.ds(pl.multiple_of(n * block, block), block)
        square = jnp.zeros((block, 1), F32)
        for ref, _step in parts:
            x = ref[at, :].astype(F32)
            square = square + jnp.sum(x * x, axis=1, keepdims=True)
        inv = lax.rsqrt(square * (1.0 / full) + NORM_EPS)
        for ref, step in parts:
            x = ref[at, :].astype(F32)
            xn_ref[:, col(step)] = (x * inv * gain_ref[:, col(step)]).astype(BF16)
        x = xn_ref[...]
        gate = dot(x, wg_ref[...])
        up = dot(x, wu_ref[...])
        hidden = (gate * (1.0 / (1.0 + jnp.exp(-gate))) * up).astype(BF16)
        for out, step in ((p2_ref, 2), (pr_ref, 1), (pl_ref, 3), (po_ref, 0)):
            out[at, :] = dot(hidden, wd_ref[:, col(step)]).astype(BF16)
        return 0

    lax.fori_loop(0, rows // block, one, 0)


def combine_body(stream_ref, weight_ref, dest_ref, *refs):
    out_ref, chunks = refs[-1], refs[:-1]
    tok = stream_ref.shape[0]
    total = stream_ref[...].astype(F32)
    for c in range(2):
        picked = None
        for k, chunk in enumerate(chunks):
            rows = chunk.shape[0]
            at = lax.broadcasted_iota(jnp.int32, (tok, rows), 1)
            d = dest_ref[:, 2 * k + c : 2 * k + c + 1]
            pick = jnp.where(at == d, 1.0, 0.0).astype(BF16)
            term = dot(pick, chunk[...])
            picked = term if picked is None else picked + term
        total = total + picked * weight_ref[:, c : c + 1]
    out_ref[...] = total.astype(BF16)


def local(
    query_proj,
    key_projection,
    value_projection,
    sink_logit,
    residual,
    w_out,
    norm_gain,
    routes,
    route_weights,
    w_gate,
    w_up,
    w_down,
):
    tok = query_proj.shape[0]
    seq = lax.axis_size("sp")
    tps = lax.axis_size("tp")
    kv = key_projection.shape[1]
    width = residual.shape[1] // tps
    sp, tp = lax.axis_index("sp"), lax.axis_index("tp")
    ids = jnp.stack([sp, tp]).astype(jnp.int32)
    to_right = [(i, (i + 1) % tps) for i in range(tps)]
    to_left = [(i, (i - 1) % tps) for i in range(tps)]

    def right(x):
        return lax.ppermute(x, "tp", to_right)

    def left(x):
        return lax.ppermute(x, "tp", to_left)

    def added(x, y):
        return (x.astype(F32) + y.astype(F32)).astype(BF16)

    def arr(rows, cols, dtype=BF16):
        return jax.ShapeDtypeStruct((rows, cols), dtype)

    tail, head = call(edges_body, [arr(WINDOW, 2 * kv)] * 2, [VMEM] * 2, 1000, "edges")(
        key_projection, value_projection
    )
    before = lax.ppermute(tail, "sp", [(i, i + 1) for i in range(seq - 1)])
    after = lax.ppermute(head, "sp", [(i + 1, i) for i in range(seq - 1)])

    experts = w_gate.shape[0] * seq
    picks = routes.T
    ids_e = jnp.arange(experts, dtype=jnp.int32)[:, None]
    hot = [(picks[c][None, :] == ids_e) for c in range(2)]
    named = (hot[0] | hot[1]).astype(BF16)
    earlier = jnp.triu(jnp.ones((tok, tok), BF16), 1)
    seen = dot(named, earlier)
    dests = []
    slots = [jnp.sum(jnp.where(h, seen, 0.0), axis=0).astype(jnp.int32) for h in hot]
    for lo, hi in CHUNKS:
        for c in range(2):
            inside = (slots[c] >= lo) & (slots[c] < hi)
            dests.append(jnp.where(inside, picks[c] * (hi - lo) + slots[c] - lo, -1))
    dest = jnp.stack(dests)

    (row_cos, col_cos), (row_sin, col_sin) = angle_tables(seq, tok)
    half = tok // 2
    p2a, p2b, pra, prb, pla, plb, po = call(
        functools.partial(attention_body, seq_devices=seq),
        [arr(half, width)] * 6 + [arr(tok, width)],
        [SMEM, SMEM] + [VMEM] * 10,
        2 * 10**9,
        "attention",
        [
            pltpu.VMEM((tok + 2 * WINDOW, 2 * HEAD_SIZE), F32),
            pltpu.VMEM((tok + 2 * WINDOW, 2 * HEAD_SIZE), F32),
            pltpu.VMEM((2, tok + 2 * WINDOW, 2 * HEAD_SIZE), BF16),
            pltpu.VMEM((2, tok + 2 * WINDOW, 2 * HEAD_SIZE), BF16),
            pltpu.VMEM((tok, query_proj.shape[1]), BF16),
        ],
    )(
        ids, sink_logit, query_proj, key_projection, value_projection, before, after,
        row_cos, row_sin, col_cos, col_sin, w_out,
    )
    a, b = right(p2a), left(p2b)
    rb, la = right(prb), left(pla)
    ra, lb = right(added(pra, a)), left(added(plb, b))
    res_cols = lax.dynamic_slice_in_dim(residual, tp * width, width, 1)
    stream, *rows_out = call(
        dispatch_body,
        [arr(tok, width)] + [arr(experts * (hi - lo), width) for lo, hi in CHUNKS],
        [VMEM] * 7,
        10**9,
        "dispatch",
    )(res_cols, po, ra, rb, la, lb, dest)

    gain = norm_gain.reshape(1, -1)
    returned = []
    for k, (lo, hi) in enumerate(CHUNKS):
        own = lax.all_to_all(
            rows_out[k].reshape(experts, hi - lo, width), "sp", 0, 0, tiled=True
        ).reshape(-1, width)
        r, l = right(own), left(own)
        far = right(r) if k % 2 == 0 else left(l)
        n = own.shape[0]
        p2, pr, pleft, pown = call(
            functools.partial(expert_body, block=256),
            [arr(n, width)] * 4,
            [SMEM] + [VMEM] * 8,
            2 * n * 2048 * 640 * 3,
            f"expert{k}",
            [pltpu.VMEM((256, 4 * width), BF16)],
        )(ids, own, r, l, far, gain, w_gate[0], w_up[0], w_down[0])
        if k % 2 == 0:
            from_left, from_right = right(added(pr, right(p2))), left(pleft)
        else:
            from_right, from_left = left(added(pleft, left(p2))), right(pr)
        summed = (
            pown.astype(F32) + from_left.astype(F32) + from_right.astype(F32)
        ).astype(BF16)
        returned.append(
            lax.all_to_all(
                summed.reshape(seq, hi - lo, width), "sp", 0, 0, tiled=True
            ).reshape(-1, width)
        )
    (out,) = call(
        combine_body, [arr(tok, width)], [VMEM] * (3 + len(CHUNKS)), 10**9, "combine"
    )(stream, route_weights, dest.T, *returned)
    return out


def solution(mesh):
    return jax.shard_map(
        local,
        mesh=mesh,
        in_specs=(
            P("sp", "tp"),
            P("sp", "tp"),
            P("sp", "tp"),
            P("tp"),
            P("sp", None),
            P("tp", None),
            P(),
            P("sp", None),
            P("sp", None),
            P("sp", None, "tp"),
            P("sp", None, "tp"),
            P("sp", "tp", None),
        ),
        out_specs=P("sp", "tp"),
        check_vma=False,
    )
```
